1024 devices in a mesh: row: 64 (over z, core), col: 16 (over y, x).
Axes of the slice: x: 4, y: 4, z: 32, core: 2. Of those that a mesh axis runs over, the one named last changes fastest.
Arguments:
- tokens: bfloat16 [32768, 2048], P('row'), may hold values from -6 to 6
- out_weight: bfloat16 [2048, 2048], P(None, 'col'), may hold values from -0.125 to 0.125
Outputs:
- mixed: bfloat16 [32768, 2048], P('row', 'col')
The draws below stay inside these ranges and needn't reach their ends.
All inputs are finite; a program needn't handle non-finite values.
Results may differ from the reference program's by a relative error of at most 0.001.
Values may be sent and summed in bfloat16 or wider, within the bound.
A program may use at most 64 MiB of HBM per device.

```python
import jax
import jax.numpy as jnp
from jax import lax

D = 2048
GROUPS = 4
GROUP_DIM = 512
LENGTH = 32768


def levels(own_key, extent, split, smallest, largest):
    def one(axis_at, parts):
        draws = jax.random.uniform(jax.random.fold_in(jax.random.fold_in(own_key, 6), axis_at), (parts,), jnp.float32, smallest / len(split), largest / len(split))
        return jnp.repeat(jnp.exp(draws), extent[axis_at] // parts).reshape((-1,) + (1,) * (len(extent) - axis_at - 1))

    factor_of = one(*split[0])
    for cut in split[1:]:
        factor_of = factor_of * one(*cut)
    return factor_of


def noise(rng, extent, width, bound, cuts=(), dtype=jnp.bfloat16):
    drawn = width * jax.random.normal(rng, extent, jnp.float32)
    if cuts:
        drawn = drawn * levels(rng, extent, cuts, -0.22, 0.18)
    return jnp.clip(drawn, -bound, bound).astype(dtype)


def setup_inputs(seed: int = 0) -> dict:
    keys = jax.random.split(jax.random.key(seed), 3)
    tokens = noise(keys[0], (LENGTH, D), 1.0, 6.0, ((0, 64),))
    out_weight = noise(keys[1], (D, D), D ** -0.5, 0.125, ((1, 16),))
    return {"tokens": tokens, "out_weight": out_weight}


def per_group(block):
    return jnp.fft.fft2(block, norm="ortho").real.astype(jnp.float32)


def reference(tokens, out_weight):
    grouped = tokens.astype(jnp.float32).reshape(LENGTH, GROUPS, GROUP_DIM)
    spectra = lax.map(per_group, jnp.moveaxis(grouped, 1, 0))
    spectral = jnp.moveaxis(spectra, 0, 1).reshape(LENGTH, D).astype(jnp.float32)
    mixed = jnp.dot(spectral, out_weight.astype(jnp.float32), precision=lax.Precision.HIGHEST, preferred_element_type=jnp.float32)
    return mixed.astype(jnp.bfloat16)
```

```python
import functools
import math

import jax
import jax.numpy as jnp
import numpy as np
from jax import lax
from jax.experimental import pallas as pl
from jax.experimental.pallas import tpu as pltpu
from jax.sharding import PartitionSpec as P

GROUPS = 4
GROUP_DIM = 512
MESH_ID = pl.DeviceIdType.MESH
BF16 = jnp.bfloat16
F32 = jnp.float32

FLOOR = 2.0**-6
LIMIT = 34800.0
SHIFT = 87.0
GAIN = 175.0 / math.log1p(LIMIT / FLOOR)


def split_table(table):
    hi = table.astype(np.float32).astype(jnp.bfloat16)
    lo = (table - hi.astype(np.float64)).astype(np.float32).astype(jnp.bfloat16)
    return hi, lo


def make_tables(row_count, seg_rows):
    length = row_count * seg_rows
    idx = np.arange(seg_rows)
    phase = (idx[:, None] * idx[None, :]) % seg_rows * (2 * np.pi / seg_rows)
    cos_hi, cos_lo = split_table(np.cos(phase))
    sin_hi, sin_lo = split_table(np.sin(phase))
    seg_table = np.concatenate([cos_hi, cos_lo, sin_hi, sin_lo], axis=0)
    row = np.arange(row_count)
    phase = (row[:, None] * row[None, :]) % row_count * (2 * np.pi / row_count)
    cos, sin = np.cos(phase), np.sin(phase)
    row_hi, row_lo = split_table(np.block([[cos, sin], [-sin, cos]]))
    row_table = np.concatenate([row_hi, row_lo], axis=0)
    phase = (row[:, None] * idx[None, :]) % length * (2 * np.pi / length)
    scaling = 1.0 / math.sqrt(length * GROUP_DIM)
    twist = np.concatenate([np.cos(phase), np.sin(phase)], axis=0) * scaling
    perm = np.zeros((256, 256), np.float32)
    for part in range(2):
        for chan in range(2):
            perm[4 * row + 2 * part + chan, part * 128 + chan * 64 + row] = 1.0
    return seg_table, row_table, twist.astype(np.float32), perm.astype(jnp.bfloat16)


def dot(a, b):
    return jnp.dot(a, b, preferred_element_type=F32)


def dot_t(a, b):
    return lax.dot_general(a, b, (((1,), (1,)), ((), ())), preferred_element_type=F32)


def halves(value):
    hi = value.astype(BF16)
    return hi, (value - hi.astype(F32)).astype(BF16)


def encode(value):
    size = jnp.exp(GAIN * jnp.log(1.0 + jnp.abs(value) * (1.0 / FLOOR)) - SHIFT)
    return jnp.where(value < 0.0, -size, size)


def decode(coded):
    size = FLOOR * (jnp.exp((jnp.log(jnp.abs(coded)) + SHIFT) * (1.0 / GAIN)) - 1.0)
    return jnp.where(coded < 0.0, -size, size)


def kernel(
    rows,
    x_hbm, w_hbm, seg_hbm, row_hbm, twist_hbm, perm_hbm, out_ref,
    x, w, seg, row_tab, twist, perm, fold, spread, send1, recv1, send2, recv2, spread2,
    load_sem, send_sem, recv_sem,
):
    me = lax.axis_index("row")
    col = lax.axis_index("col")
    chips = rows // 2
    chip = me // 2
    core = lax.rem(me, 2)

    loads = []
    for i, (src, dst) in enumerate(
        [(w_hbm, w), (seg_hbm, seg), (x_hbm, x), (perm_hbm, perm), (row_hbm, row_tab), (twist_hbm, twist)]
    ):
        load = pltpu.make_async_copy(src, dst, load_sem.at[i])
        load.start()
        loads.append(load)

    barrier = pltpu.get_barrier_semaphore()

    def greet(i, carry):
        pl.semaphore_signal(
            barrier, inc=1, device_id=(lax.rem(me + i, rows), col), device_id_type=MESH_ID
        )
        return carry

    lax.fori_loop(1, rows, greet, 0)

    def exchange(src, dst, which):
        def one(step, target_core):
            target = lax.rem(chip + step + chips, chips) * 2 + target_core
            pltpu.make_async_remote_copy(
                src_ref=src.at[target],
                dst_ref=dst.at[me],
                send_sem=send_sem.at[which],
                recv_sem=recv_sem.at[which],
                device_id=(target, col),
                device_id_type=MESH_ID,
            ).start()

        half = chips // 2
        one(half, core)
        one(half, 1 - core)

        def ring(i, carry):
            hop = half - 1 - i
            one(hop, core)
            one(-hop, core)
            one(hop, 1 - core)
            one(-hop, 1 - core)
            return carry

        lax.fori_loop(0, half - 1, ring, 0)
        one(0, 1 - core)
        dst[pl.ds(me, 1)] = src[pl.ds(me, 1)]

    def arrived(dst, which):
        part = dst.at[pl.ds(0, rows - 1)]
        pltpu.make_async_copy(part, part, recv_sem.at[which]).wait()

    def departed(src, which):
        part = src.at[pl.ds(0, rows - 1)]
        pltpu.make_async_copy(part, part, send_sem.at[which]).wait()

    loads[0].wait()
    loads[1].wait()
    wide = jnp.concatenate([w[g * 512 : (g + 1) * 512, :] for g in range(GROUPS)], axis=1)
    for part in range(2):
        sign = 1.0 - 2.0 * part
        base = part * 1024
        folded = (dot(seg[base : base + 512, :], wide) + dot(seg[base + 512 : base + 1024, :], wide)) * sign
        hi, lo = halves(folded)
        for g in range(GROUPS):
            fold[g * 512 : (g + 1) * 512, part * 128 : (part + 1) * 128] = hi[:, g * 128 : (g + 1) * 128]
            fold[g * 512 : (g + 1) * 512, 256 + part * 128 : 256 + (part + 1) * 128] = lo[:, g * 128 : (g + 1) * 128]

    loads[2].wait()
    loads[3].wait()
    both = dot(x[...], fold[...])
    coded = encode(both[:, :256] + both[:, 256:]).astype(BF16)
    for q in range(4):
        turned = dot_t(perm[...], coded[q * 128 : (q + 1) * 128, :])
        spread[pl.ds(q, 256, stride=4), :] = turned
    send1[...] = spread[...].astype(BF16).reshape(rows, 16, 128)

    pl.semaphore_wait(barrier, rows - 1)
    exchange(send1, recv1, 0)
    loads[4].wait()
    loads[5].wait()
    arrived(recv1, 0)

    spread[...] = decode(recv1[...].reshape(rows * 16, 128).astype(F32))
    parts = []
    for part in range(2):
        parts.append(
            jnp.concatenate(
                [spread[pl.ds(part * 8 + u, rows, stride=16), :] for u in range(8)], axis=1
            )
        )
    hi, lo = halves(jnp.concatenate(parts, axis=0))
    first = dot(row_tab[:128, :], hi) + dot(row_tab[:128, :], lo) + dot(row_tab[128:, :], hi)
    tc = twist[:rows, :]
    ts = twist[rows:, :]
    real, imag = [], []
    for c in range(2):
        re = first[:rows, c * 512 : (c + 1) * 512]
        im = first[rows:, c * 512 : (c + 1) * 512]
        real.append(tc * re + ts * im)
        imag.append(tc * im - ts * re)
    re_hi, re_lo = halves(jnp.concatenate(real, axis=0))
    im_hi, im_lo = halves(jnp.concatenate(imag, axis=0))
    res = dot_t(seg[0:512, :], re_hi) + dot_t(seg[0:512, :], re_lo) + dot_t(seg[512:1024, :], re_hi)
    res = res + dot_t(seg[1024:1536, :], im_hi) + dot_t(seg[1024:1536, :], im_lo) + dot_t(seg[1536:2048, :], im_hi)
    send2[...] = res.reshape(rows, 8, 128).astype(BF16)
    exchange(send2, recv2, 1)
    arrived(recv2, 1)

    spread2[...] = recv2[...].astype(F32).reshape(rows * 8, 128)
    low = lax.broadcasted_iota(jnp.int32, (rows, 128), 1) < 64
    for pair in range(4):
        even = spread2[pl.ds(2 * pair, rows, stride=8), :]
        odd = spread2[pl.ds(2 * pair + 1, rows, stride=8), :]
        top = jnp.where(low, even, pltpu.roll(odd, 64, 1))
        bottom = jnp.where(low, pltpu.roll(even, 64, 1), odd)
        turned = jnp.concatenate([top, bottom], axis=0).T
        out_ref[pair * 128 : (pair + 1) * 128, :] = turned.astype(BF16)
    departed(send1, 0)
    departed(send2, 1)


def body(tokens, out_weight):
    rows = lax.axis_size("row")
    seg_rows = tokens.shape[0]
    tables = [jnp.asarray(t) for t in make_tables(rows, seg_rows)]
    operands = [tokens, out_weight] + tables
    scratch = [pltpu.VMEM(a.shape, a.dtype) for a in operands]
    scratch += [
        pltpu.VMEM((2048, 512), BF16),
        pltpu.VMEM((rows * 16, 128), F32),
        pltpu.VMEM((rows, 16, 128), BF16),
        pltpu.VMEM((rows, 16, 128), BF16),
        pltpu.VMEM((rows, 8, 128), BF16),
        pltpu.VMEM((rows, 8, 128), BF16),
        pltpu.VMEM((rows * 8, 128), F32),
        pltpu.SemaphoreType.DMA((6,)),
        pltpu.SemaphoreType.DMA((2,)),
        pltpu.SemaphoreType.DMA((2,)),
    ]
    return pl.pallas_call(
        functools.partial(kernel, rows),
        out_shape=jax.ShapeDtypeStruct((seg_rows, out_weight.shape[1]), BF16),
        in_specs=[pl.BlockSpec(memory_space=pl.ANY)] * len(operands),
        out_specs=pl.BlockSpec(memory_space=pltpu.VMEM),
        scratch_shapes=scratch,
        compiler_params=pltpu.CompilerParams(
            collective_id=0, has_side_effects=True, vmem_limit_bytes=60 * 1024 * 1024
        ),
        name="mix",
    )(*operands)


def solution(mesh):
    placed = (P("row", None), P(None, "col"))
    return jax.shard_map(
        body, mesh=mesh, in_specs=placed, out_specs=P("row", "col"), check_vma=False
    )
```

```python
import functools
import math

import jax
import jax.numpy as jnp
import numpy as np
from jax import lax
from jax.experimental import pallas as pl
from jax.experimental.pallas import tpu as pltpu
from jax.sharding import PartitionSpec as P

GROUPS = 4
GROUP_DIM = 512
MESH_ID = pl.DeviceIdType.MESH
BF16 = jnp.bfloat16
F32 = jnp.float32

FLOOR = 2.0**-6
LIMIT = 34800.0
SHIFT = 87.0
GAIN = 175.0 / math.log1p(LIMIT / FLOOR)


EARLY = ((8, 1),)
LATE = ((16, 9),)


def split_table(table):
    hi = table.astype(np.float32).astype(jnp.bfloat16)
    lo = (table - hi.astype(np.float64)).astype(np.float32).astype(jnp.bfloat16)
    return hi, lo


def make_tables(row_count, seg_rows):
    length = row_count * seg_rows
    idx = np.arange(seg_rows)
    phase = (idx[:, None] * idx[None, :]) % seg_rows * (2 * np.pi / seg_rows)
    cos_hi, cos_lo = split_table(np.cos(phase))
    sin_hi, sin_lo = split_table(np.sin(phase))
    row = np.arange(row_count)
    phase = (row[:, None] * row[None, :]) % row_count * (2 * np.pi / row_count)
    cos, sin = np.cos(phase), np.sin(phase)
    row_hi, row_lo = split_table(np.block([[cos, sin], [-sin, cos]]))
    phase = (row[:, None] * idx[None, :]) % length * (2 * np.pi / length)
    scaling = 1.0 / math.sqrt(length * GROUP_DIM)
    twist_hi, twist_lo = split_table(np.concatenate([np.cos(phase), np.sin(phase)], axis=0) * scaling)
    mixed = np.zeros((512, 512), jnp.bfloat16)
    for part in range(2):
        for chan in range(2):
            own = 8 * (row // 2) + 4 * (row % 2) + 2 * part + chan
            swapped = 8 * (row // 2) + 4 * (1 - row % 2) + 2 * part + chan
            source = part * 128 + chan * 64 + row
            mixed[own, source] = 1.0
            mixed[256 + swapped, source] = 1.0
    mixed[:, 256:384] = np.concatenate([row_hi, row_lo, row_hi, row_lo], axis=0)
    return np.concatenate([cos_hi, cos_lo, sin_hi, sin_lo, twist_hi, twist_lo, mixed], axis=0)


def dot(a, b):
    return jnp.dot(a, b, preferred_element_type=F32)


def dot_t(a, b):
    return lax.dot_general(a, b, (((1,), (1,)), ((), ())), preferred_element_type=F32)


def halves(value):
    hi = value.astype(BF16)
    return hi, (value - hi.astype(F32)).astype(BF16)


def encode(value):
    size = jnp.exp(GAIN * jnp.log(1.0 + jnp.abs(value) * (1.0 / FLOOR)) - SHIFT)
    return jnp.where(value < 0.0, -size, size)


def decode(coded):
    size = FLOOR * (jnp.exp((jnp.log(jnp.abs(coded)) + SHIFT) * (1.0 / GAIN)) - 1.0)
    return jnp.where(coded < 0.0, -size, size)


def kernel(
    rows,
    x_hbm, w_hbm, tab_hbm, out_ref,
    x, w, tab, fold, spread, send1, recv1, send2, recv2, spread2,
    load_sem, send_sem, recv_sem, word_sem,
):
    me = lax.axis_index("row")
    col = lax.axis_index("col")
    chips = rows // 2
    chip = me // 2
    core = lax.rem(me, 2)

    loads = []
    for i, (src, dst) in enumerate(
        [
            (w_hbm, w),
            (tab_hbm.at[0:1024], tab.at[0:1024]),
            (tab_hbm.at[1024:2048], tab.at[1024:2048]),
            (x_hbm, x),
            (tab_hbm.at[2048:2816], tab.at[2048:2816]),
        ]
    ):
        load = pltpu.make_async_copy(src, dst, load_sem.at[i])
        load.start()
        loads.append(load)

    barrier = pltpu.get_barrier_semaphore()
    reach = chips // 4

    def place(step, target_core):
        return lax.rem(chip + step + chips, chips) * 2 + target_core

    def signal(sem, step, target_core):
        pl.semaphore_signal(
            sem, inc=1, device_id=(place(step, target_core), col), device_id_type=MESH_ID
        )

    signal(barrier, 0, 1 - core)

    def greet(i, carry):
        for step in (reach - i, i - reach):
            signal(barrier, step, core)
            signal(barrier, step, 1 - core)
        return carry

    lax.fori_loop(0, reach, greet, 0)

    def known_near():
        pl.semaphore_wait(barrier, 4 * reach + 1)
        signal(word_sem, reach, core)
        signal(word_sem, -reach, core)

    def known_all():
        pl.semaphore_wait(word_sem, 2)

    def send(src, dst, which, step, target_core):
        target_chip = lax.rem(chip + step + chips, chips)
        pltpu.make_async_remote_copy(
            src_ref=src.at[target_chip, target_core],
            dst_ref=dst.at[me],
            send_sem=send_sem.at[which],
            recv_sem=recv_sem.at[which],
            device_id=(target_chip * 2 + target_core, col),
            device_id_type=MESH_ID,
        ).start()

    def send_ring(src, dst, which, far, near):
        if far == chips // 2:
            send(src, dst, which, far, core)
            send(src, dst, which, far, 1 - core)
            far -= 1

        def ring(i, carry):
            hop = far - i
            for target_core in (core, 1 - core):
                send(src, dst, which, hop, target_core)
                send(src, dst, which, -hop, target_core)
            return carry

        lax.fori_loop(0, far - near + 1, ring, 0)

    def keep_own(src, dst):
        dst[pl.ds(me, 1)] = src[pl.ds(chip, 1), pl.ds(core, 1)][0]

    def arrived(dst, which):
        part = dst.at[pl.ds(0, rows - 1)]
        pltpu.make_async_copy(part, part, recv_sem.at[which]).wait()

    def departed(dst, which):
        part = dst.at[pl.ds(0, rows - 1)]
        pltpu.make_async_copy(part, part, send_sem.at[which]).wait()

    loads[0].wait()
    wide = jnp.concatenate([w[g * 512 : (g + 1) * 512, :] for g in range(GROUPS)], axis=1)
    for part in range(2):
        loads[1 + part].wait()
        base = part * 1024
        folded = dot(tab[base : base + 512, :], wide) + dot(tab[base + 512 : base + 1024, :], wide)
        hi, lo = halves(-folded if part else folded)
        for g in range(GROUPS):
            fold[g * 512 : (g + 1) * 512, part * 128 : (part + 1) * 128] = hi[:, g * 128 : (g + 1) * 128]
            fold[g * 512 : (g + 1) * 512, 256 + part * 128 : 256 + (part + 1) * 128] = lo[:, g * 128 : (g + 1) * 128]

    loads[3].wait()
    both = dot(x[...], fold[...])
    coded = encode(both[:, :256] + both[:, 256:]).astype(BF16)
    loads[4].wait()
    own = dot_t(tab[2304:2560, 0:256], coded).reshape(rows // 2, 8, 512)
    swapped = dot_t(tab[2560:2816, 0:256], coded).reshape(rows // 2, 8, 512)
    upper = lax.broadcasted_iota(jnp.int32, (rows // 2, 8, 128), 1) < 4
    for parity, (one, two) in enumerate(((own, swapped), (swapped, own))):
        for half in range(2):
            lanes = half * 256
            block = jnp.where(upper, one[:, :, lanes : lanes + 128], two[:, :, lanes + 128 : lanes + 256])
            send1[:, parity, half * 8 : (half + 1) * 8, :] = block.astype(BF16)

    known_near()
    for far, near in EARLY:
        send_ring(send1, recv1, 0, far, near)
    known_all()
    for far, near in LATE:
        send_ring(send1, recv1, 0, far, near)
    send(send1, recv1, 0, 0, 1 - core)
    keep_own(send1, recv1)
    arrived(recv1, 0)

    spread[...] = decode(recv1[...].reshape(rows * 16, 128).astype(F32))
    parts = []
    for part in range(2):
        parts.append(
            jnp.concatenate(
                [
                    spread[pl.ds(4 * q + 2 * part + c, rows, stride=16), :]
                    for c in range(2)
                    for q in range(4)
                ],
                axis=1,
            )
        )
    hi, lo = halves(jnp.concatenate(parts, axis=0))
    row_hi = tab[2304:2432, 256:384]
    first = dot(row_hi, hi) + dot(row_hi, lo) + dot(tab[2432:2560, 256:384], hi)
    twist = tab[2048:2176, :].astype(F32) + tab[2176:2304, :].astype(F32)
    tc = twist[:rows, :]
    ts = twist[rows:, :]
    real, imag = [], []
    for c in range(2):
        re = first[:rows, c * 512 : (c + 1) * 512]
        im = first[rows:, c * 512 : (c + 1) * 512]
        real.append(tc * re + ts * im)
        imag.append(tc * im - ts * re)
    re_hi, re_lo = halves(jnp.concatenate(real, axis=0))
    im_hi, im_lo = halves(jnp.concatenate(imag, axis=0))
    res = dot_t(tab[0:512, :], re_hi) + dot_t(tab[0:512, :], re_lo) + dot_t(tab[512:1024, :], re_hi)
    res = res + dot_t(tab[1024:1536, :], im_hi) + dot_t(tab[1024:1536, :], im_lo) + dot_t(tab[1536:2048, :], im_hi)
    send2[...] = res.reshape(rows // 2, 2, 8, 128).astype(BF16)
    send_ring(send2, recv2, 1, 16, 1)
    send(send2, recv2, 1, 0, 1 - core)
    keep_own(send2, recv2)
    arrived(recv2, 1)

    spread2[...] = recv2[...].astype(F32).reshape(rows * 8, 128)
    low = lax.broadcasted_iota(jnp.int32, (rows, 128), 1) < 64
    for pair in range(4):
        even = spread2[pl.ds(2 * pair, rows, stride=8), :]
        odd = spread2[pl.ds(2 * pair + 1, rows, stride=8), :]
        top = jnp.where(low, even, pltpu.roll(odd, 64, 1))
        bottom = jnp.where(low, pltpu.roll(even, 64, 1), odd)
        turned = jnp.concatenate([top, bottom], axis=0).T
        out_ref[pair * 128 : (pair + 1) * 128, :] = turned.astype(BF16)
    departed(recv1, 0)
    departed(recv2, 1)


def body(tokens, out_weight):
    rows = lax.axis_size("row")
    seg_rows = tokens.shape[0]
    operands = [tokens, out_weight, jnp.asarray(make_tables(rows, seg_rows))]
    scratch = [pltpu.VMEM(a.shape, a.dtype) for a in operands]
    scratch += [
        pltpu.VMEM((2048, 512), BF16),
        pltpu.VMEM((rows * 16, 128), F32),
        pltpu.VMEM((rows // 2, 2, 16, 128), BF16),
        pltpu.VMEM((rows, 16, 128), BF16),
        pltpu.VMEM((rows // 2, 2, 8, 128), BF16),
        pltpu.VMEM((rows, 8, 128), BF16),
        pltpu.VMEM((rows * 8, 128), F32),
        pltpu.SemaphoreType.DMA((5,)),
        pltpu.SemaphoreType.DMA((2,)),
        pltpu.SemaphoreType.DMA((2,)),
        pltpu.SemaphoreType.REGULAR,
    ]
    return pl.pallas_call(
        functools.partial(kernel, rows),
        out_shape=jax.ShapeDtypeStruct((seg_rows, out_weight.shape[1]), BF16),
        in_specs=[pl.BlockSpec(memory_space=pl.ANY)] * len(operands),
        out_specs=pl.BlockSpec(memory_space=pltpu.VMEM),
        scratch_shapes=scratch,
        compiler_params=pltpu.CompilerParams(
            collective_id=0, has_side_effects=True, vmem_limit_bytes=54848 * 1024
        ),
        name="mix",
    )(*operands)


def solution(mesh):
    placed = (P("row", None), P(None, "col"))
    return jax.shard_map(
        body, mesh=mesh, in_specs=placed, out_specs=P("row", "col"), check_vma=False
    )
```

```python
import functools
import math

import jax
import jax.numpy as jnp
import numpy as np
from jax import lax
from jax.experimental import pallas as pl
from jax.experimental.pallas import tpu as pltpu
from jax.sharding import PartitionSpec as P

GROUPS = 4
GROUP_DIM = 512
MESH_ID = pl.DeviceIdType.MESH
BF16 = jnp.bfloat16
F32 = jnp.float32

FLOOR = 2.0**-6
LIMIT = 34800.0
SHIFT = 87.0
GAIN = 175.0 / math.log1p(LIMIT / FLOOR)


def split_table(table):
    hi = table.astype(np.float32).astype(jnp.bfloat16)
    lo = (table - hi.astype(np.float64)).astype(np.float32).astype(jnp.bfloat16)
    return hi, lo


def make_tables(row_count, seg_rows):
    length = row_count * seg_rows
    idx = np.arange(seg_rows)
    phase = (idx[:, None] * idx[None, :]) % seg_rows * (2 * np.pi / seg_rows)
    cos_hi, cos_lo = split_table(np.cos(phase))
    sin_hi, sin_lo = split_table(np.sin(phase))
    row = np.arange(row_count)
    phase = (row[:, None] * row[None, :]) % row_count * (2 * np.pi / row_count)
    cos, sin = np.cos(phase), np.sin(phase)
    row_hi, row_lo = split_table(np.block([[cos, sin], [-sin, cos]]))
    phase = (row[:, None] * idx[None, :]) % length * (2 * np.pi / length)
    scaling = 1.0 / math.sqrt(length * GROUP_DIM)
    twist_hi, twist_lo = split_table(np.concatenate([np.cos(phase), np.sin(phase)], axis=0) * scaling)
    mixed = np.zeros((256, 512), jnp.bfloat16)
    for part in range(2):
        for chan in range(2):
            mixed[128 * chan + 2 * row + part, part * 128 + chan * 64 + row] = 1.0
    mixed[:, 256:384] = np.concatenate([row_hi, row_lo], axis=0)
    return np.concatenate([cos_hi, cos_lo, sin_hi, sin_lo, twist_hi, twist_lo, mixed], axis=0)


def dot(a, b):
    return jnp.dot(a, b, preferred_element_type=F32)


def dot_t(a, b):
    return lax.dot_general(a, b, (((1,), (1,)), ((), ())), preferred_element_type=F32)


def halves(value):
    hi = value.astype(BF16)
    return hi, (value - hi.astype(F32)).astype(BF16)


def encode(value):
    size = jnp.exp(GAIN * jnp.log(1.0 + jnp.abs(value) * (1.0 / FLOOR)) - SHIFT)
    return jnp.where(value < 0.0, -size, size)


def decode(coded):
    size = FLOOR * (jnp.exp((jnp.log(jnp.abs(coded)) + SHIFT) * (1.0 / GAIN)) - 1.0)
    return jnp.where(coded < 0.0, -size, size)


def kernel(
    rows,
    x_hbm, w_hbm, tab_hbm, out_ref,
    x, w, tab, fold, spread, send1, recv1, send2, recv2, spread2,
    load_sem, send_sem, recv_sem, word_sem,
):
    me = lax.axis_index("row")
    col = lax.axis_index("col")
    chips = rows // 2
    chip = me // 2
    core = lax.rem(me, 2)

    loads = []
    for i, (src, dst) in enumerate(
        [
            (w_hbm, w),
            (tab_hbm.at[0:1024], tab.at[0:1024]),
            (tab_hbm.at[1024:2048], tab.at[1024:2048]),
            (x_hbm, x),
            (tab_hbm.at[2048:2560], tab.at[2048:2560]),
        ]
    ):
        load = pltpu.make_async_copy(src, dst, load_sem.at[i])
        load.start()
        loads.append(load)

    barrier = pltpu.get_barrier_semaphore()
    reach = chips // 4

    def place(step, target_core):
        return lax.rem(chip + step + chips, chips) * 2 + target_core

    def signal(sem, step, target_core):
        pl.semaphore_signal(
            sem, inc=1, device_id=(place(step, target_core), col), device_id_type=MESH_ID
        )

    signal(barrier, 0, 1 - core)

    def greet(i, carry):
        for step in (reach - i, i - reach):
            signal(barrier, step, core)
            signal(barrier, step, 1 - core)
        return carry

    lax.fori_loop(0, reach, greet, 0)

    def known_near():
        pl.semaphore_wait(barrier, 4 * reach + 1)
        signal(word_sem, reach, core)
        signal(word_sem, -reach, core)

    def known_all():
        pl.semaphore_wait(word_sem, 2)

    def send(src, dst, which, step, target_core):
        target_chip = lax.rem(chip + step + chips, chips)
        pltpu.make_async_remote_copy(
            src_ref=src.at[target_chip, target_core],
            dst_ref=dst.at[me],
            send_sem=send_sem.at[which],
            recv_sem=recv_sem.at[which],
            device_id=(target_chip * 2 + target_core, col),
            device_id_type=MESH_ID,
        ).start()

    def send_ring(src, dst, which, far, near):
        if far == chips // 2:
            send(src, dst, which, far, core)
            send(src, dst, which, far, 1 - core)
            far -= 1

        def ring(i, carry):
            hop = far - i
            for target_core in (core, 1 - core):
                send(src, dst, which, hop, target_core)
                send(src, dst, which, -hop, target_core)
            return carry

        lax.fori_loop(0, far - near + 1, ring, 0)

    def keep_own(src, dst, c):
        dst[c, pl.ds(me, 1)] = src[c, pl.ds(chip, 1), pl.ds(core, 1)][0]

    def arrived(dst, which):
        part = dst.at[pl.ds(0, rows - 1)]
        pltpu.make_async_copy(part, part, recv_sem.at[which]).wait()

    def departed(dst, which):
        part = dst.at[pl.ds(0, rows - 1)]
        pltpu.make_async_copy(part, part, send_sem.at[which]).wait()

    loads[0].wait()
    wide = jnp.concatenate([w[g * 512 : (g + 1) * 512, :] for g in range(GROUPS)], axis=1)
    for part in range(2):
        loads[1 + part].wait()
        base = part * 1024
        folded = dot(tab[base : base + 512, :], wide) + dot(tab[base + 512 : base + 1024, :], wide)
        hi, lo = halves(-folded if part else folded)
        for g in range(GROUPS):
            fold[g * 512 : (g + 1) * 512, part * 128 : (part + 1) * 128] = hi[:, g * 128 : (g + 1) * 128]
            fold[g * 512 : (g + 1) * 512, 256 + part * 128 : 256 + (part + 1) * 128] = lo[:, g * 128 : (g + 1) * 128]

    loads[3].wait()
    both = dot(x[...], fold[...])
    coded = encode(both[:, :256] + both[:, 256:]).astype(BF16)
    loads[4].wait()
    for q in range(4):
        turned = dot_t(tab[2304:2560, 0:256], coded[q * 128 : (q + 1) * 128, :])
        spread[pl.ds(q, 256, stride=4), :] = turned
    send1[...] = spread[...].astype(BF16).reshape(2, rows // 2, 2, 8, 128)

    known_near()
    for c in range(2):
        send_ring(send1.at[c], recv1.at[c], c, 8, 1)
    known_all()
    for c in range(2):
        send_ring(send1.at[c], recv1.at[c], c, 16, 9)
        send(send1.at[c], recv1.at[c], c, 0, 1 - core)
        keep_own(send1, recv1, c)

    twist = tab[2048:2176, :].astype(F32) + tab[2176:2304, :].astype(F32)
    tc = twist[:rows, :]
    ts = twist[rows:, :]
    row_hi = tab[2304:2432, 256:384]
    row_lo = tab[2432:2560, 256:384]
    low = lax.broadcasted_iota(jnp.int32, (256, 128), 1) < 64
    for c in range(2):
        arrived(recv1.at[c], c)
        base = c * 512
        spread[base : base + 512, :] = decode(recv1[c].astype(F32).reshape(rows * 8, 128))
        parts = []
        for part in range(2):
            parts.append(
                jnp.concatenate(
                    [spread[pl.ds(base + 4 * part + q, rows, stride=8), :] for q in range(4)], axis=1
                )
            )
        hi, lo = halves(jnp.concatenate(parts, axis=0))
        first = dot(row_hi, hi) + dot(row_hi, lo) + dot(row_lo, hi)
        re = first[:rows, :]
        im = first[rows:, :]
        re_hi, re_lo = halves(tc * re + ts * im)
        im_hi, im_lo = halves(tc * im - ts * re)
        res = dot_t(tab[512:1024, :], jnp.concatenate([re_hi, re_hi], axis=0))
        res = res + dot_t(tab[1536:2048, :], jnp.concatenate([im_hi, im_hi], axis=0))
        both = dot_t(tab[0:512, :], jnp.concatenate([re_hi, re_hi, re_lo, re_lo], axis=0))
        both = both + dot_t(tab[1024:1536, :], jnp.concatenate([im_hi, im_hi, im_lo, im_lo], axis=0))
        spread2[...] = res + both[:, :128] + both[:, 128:]
        paired = jnp.where(low, spread2[pl.ds(0, 256, stride=2), :], spread2[pl.ds(1, 256, stride=2), :])
        send2[c] = paired.reshape(rows // 2, 2, 4, 128).astype(BF16)
        send_ring(send2.at[c], recv2.at[c], 2 + c, 16, 1)
        send(send2.at[c], recv2.at[c], 2 + c, 0, 1 - core)
        keep_own(send2, recv2, c)

    for c in range(2):
        arrived(recv2.at[c], 2 + c)
        spread2[c * 256 : (c + 1) * 256, :] = recv2[c].astype(F32).reshape(rows * 4, 128)
    for pair in range(4):
        turned = jnp.concatenate(
            [spread2[pl.ds(c * 256 + pair, rows, stride=4), :] for c in range(2)], axis=0
        ).T
        out_ref[pair * 128 : (pair + 1) * 128, :] = turned.astype(BF16)
    for c in range(2):
        departed(recv1.at[c], c)
        departed(recv2.at[c], 2 + c)


def body(tokens, out_weight):
    rows = lax.axis_size("row")
    seg_rows = tokens.shape[0]
    operands = [tokens, out_weight, jnp.asarray(make_tables(rows, seg_rows))]
    scratch = [pltpu.VMEM(a.shape, a.dtype) for a in operands]
    scratch += [
        pltpu.VMEM((2048, 512), BF16),
        pltpu.VMEM((rows * 16, 128), F32),
        pltpu.VMEM((2, rows // 2, 2, 8, 128), BF16),
        pltpu.VMEM((2, rows, 8, 128), BF16),
        pltpu.VMEM((2, rows // 2, 2, 4, 128), BF16),
        pltpu.VMEM((2, rows, 4, 128), BF16),
        pltpu.VMEM((rows * 8, 128), F32),
        pltpu.SemaphoreType.DMA((5,)),
        pltpu.SemaphoreType.DMA((4,)),
        pltpu.SemaphoreType.DMA((4,)),
        pltpu.SemaphoreType.REGULAR,
    ]
    return pl.pallas_call(
        functools.partial(kernel, rows),
        out_shape=jax.ShapeDtypeStruct((seg_rows, out_weight.shape[1]), BF16),
        in_specs=[pl.BlockSpec(memory_space=pl.ANY)] * len(operands),
        out_specs=pl.BlockSpec(memory_space=pltpu.VMEM),
        scratch_shapes=scratch,
        compiler_params=pltpu.CompilerParams(
            collective_id=0, has_side_effects=True, vmem_limit_bytes=54848 * 1024
        ),
        name="mix",
    )(*operands)


def solution(mesh):
    placed = (P("row", None), P(None, "col"))
    return jax.shard_map(
        body, mesh=mesh, in_specs=placed, out_specs=P("row", "col"), check_vma=False
    )
```

```python
import functools
import math

import jax
import jax.numpy as jnp
import numpy as np
from jax import lax
from jax.experimental import pallas as pl
from jax.experimental.pallas import tpu as pltpu
from jax.sharding import PartitionSpec as P

GROUPS = 4
GROUP_DIM = 512
MESH_ID = pl.DeviceIdType.MESH
BF16 = jnp.bfloat16
F32 = jnp.float32

FLOOR = 2.0**-6
LIMIT = 34800.0
SHIFT = 87.0
GAIN = 175.0 / math.log1p(LIMIT / FLOOR)


def split_table(table):
    hi = table.astype(np.float32).astype(jnp.bfloat16)
    lo = (table - hi.astype(np.float64)).astype(np.float32).astype(jnp.bfloat16)
    return hi, lo


def make_tables(row_count, seg_rows):
    length = row_count * seg_rows
    idx = np.arange(seg_rows)
    phase = (idx[:, None] * idx[None, :]) % seg_rows * (2 * np.pi / seg_rows)
    cos_hi, cos_lo = split_table(np.cos(phase))
    sin_hi, sin_lo = split_table(np.sin(phase))
    row = np.arange(row_count)
    phase = (row[:, None] * row[None, :]) % row_count * (2 * np.pi / row_count)
    cos, sin = np.cos(phase), np.sin(phase)
    row_hi, row_lo = split_table(np.block([[cos, sin], [-sin, cos]]))
    phase = (row[:, None] * idx[None, :]) % length * (2 * np.pi / length)
    scaling = 1.0 / math.sqrt(length * GROUP_DIM)
    twist_hi, twist_lo = split_table(np.concatenate([np.cos(phase), np.sin(phase)], axis=0) * scaling)
    mixed = np.zeros((256, 512), jnp.bfloat16)
    for part in range(2):
        for chan in range(2):
            mixed[128 * chan + 2 * row + part, part * 128 + chan * 64 + row] = 1.0
    mixed[:, 256:384] = np.concatenate([row_hi, row_lo], axis=0)
    return np.concatenate([cos_hi, cos_lo, sin_hi, sin_lo, twist_hi, twist_lo, mixed], axis=0)


def dot(a, b):
    return jnp.dot(a, b, preferred_element_type=F32)


def dot_t(a, b):
    return lax.dot_general(a, b, (((1,), (1,)), ((), ())), preferred_element_type=F32)


def halves(value):
    hi = value.astype(BF16)
    return hi, (value - hi.astype(F32)).astype(BF16)


def encode(value):
    size = jnp.exp(GAIN * jnp.log(1.0 + jnp.abs(value) * (1.0 / FLOOR)) - SHIFT)
    return jnp.where(value < 0.0, -size, size)


def decode(coded):
    size = FLOOR * (jnp.exp((jnp.log(jnp.abs(coded)) + SHIFT) * (1.0 / GAIN)) - 1.0)
    return jnp.where(coded < 0.0, -size, size)


def kernel(
    rows,
    x_hbm, w_hbm, tab_hbm, out_ref,
    x, w, tab, fold, spread, send1, recv1, send2, recv2, spread2,
    load_sem, send_sem, recv_sem, word_sem,
):
    me = lax.axis_index("row")
    col = lax.axis_index("col")
    chips = rows // 2
    chip = me // 2
    core = lax.rem(me, 2)

    loads = []
    for i, (src, dst) in enumerate(
        [
            (w_hbm, w),
            (tab_hbm.at[0:1024], tab.at[0:1024]),
            (tab_hbm.at[1024:2048], tab.at[1024:2048]),
            (x_hbm, x),
            (tab_hbm.at[2048:2560], tab.at[2048:2560]),
        ]
    ):
        load = pltpu.make_async_copy(src, dst, load_sem.at[i])
        load.start()
        loads.append(load)

    barrier = pltpu.get_barrier_semaphore()
    reach = chips // 4

    def place(step, target_core):
        return lax.rem(chip + step + chips, chips) * 2 + target_core

    def signal(sem, step, target_core):
        pl.semaphore_signal(
            sem, inc=1, device_id=(place(step, target_core), col), device_id_type=MESH_ID
        )

    signal(barrier, 0, 1 - core)

    def greet(i, carry):
        for step in (reach - i, i - reach):
            signal(barrier, step, core)
            signal(barrier, step, 1 - core)
        return carry

    lax.fori_loop(0, reach, greet, 0)

    def known_near():
        pl.semaphore_wait(barrier, 4 * reach + 1)
        signal(word_sem, reach, core)
        signal(word_sem, -reach, core)

    def known_all():
        pl.semaphore_wait(word_sem, 2)

    def send(src, dst, which, step, target_core):
        target_chip = lax.rem(chip + step + chips, chips)
        pltpu.make_async_remote_copy(
            src_ref=src.at[target_chip, target_core],
            dst_ref=dst.at[me],
            send_sem=send_sem.at[which],
            recv_sem=recv_sem.at[which],
            device_id=(target_chip * 2 + target_core, col),
            device_id_type=MESH_ID,
        ).start()

    def send_ring(src, dst, which, far, near):
        if far == chips // 2:
            send(src, dst, which, far, core)
            send(src, dst, which, far, 1 - core)
            far -= 1

        def ring(i, carry):
            hop = far - i
            for target_core in (core, 1 - core):
                send(src, dst, which, hop, target_core)
                send(src, dst, which, -hop, target_core)
            return carry

        lax.fori_loop(0, far - near + 1, ring, 0)

    def keep_own(src, dst, c):
        dst[c, pl.ds(me, 1)] = src[c, pl.ds(chip, 1), pl.ds(core, 1)][0]

    def arrived(dst, which):
        part = dst.at[pl.ds(0, rows - 1)]
        pltpu.make_async_copy(part, part, recv_sem.at[which]).wait()

    def departed(dst, which):
        part = dst.at[pl.ds(0, rows - 1)]
        pltpu.make_async_copy(part, part, send_sem.at[which]).wait()

    loads[0].wait()
    wide = jnp.concatenate([w[g * 512 : (g + 1) * 512, :] for g in range(GROUPS)], axis=1)
    for part in range(2):
        loads[1 + part].wait()
        base = part * 1024
        folded = dot(tab[base : base + 512, :], wide) + dot(tab[base + 512 : base + 1024, :], wide)
        hi, lo = halves(-folded if part else folded)
        for g in range(GROUPS):
            fold[g * 512 : (g + 1) * 512, part * 128 : (part + 1) * 128] = hi[:, g * 128 : (g + 1) * 128]
            fold[g * 512 : (g + 1) * 512, 256 + part * 128 : 256 + (part + 1) * 128] = lo[:, g * 128 : (g + 1) * 128]

    loads[3].wait()
    both = dot(x[...], fold[...])
    coded = encode(both[:, :256] + both[:, 256:]).astype(BF16)
    loads[4].wait()
    for q in range(4):
        turned = dot_t(tab[2304:2560, 0:256], coded[q * 128 : (q + 1) * 128, :])
        spread[pl.ds(q, 256, stride=4), :] = turned
    send1[...] = spread[...].astype(BF16).reshape(2, rows // 2, 2, 8, 128)

    known_near()
    send_ring(send1.at[0], recv1.at[0], 0, 8, 1)
    send_ring(send1.at[1], recv1.at[1], 1, 8, 5)
    known_all()
    send_ring(send1.at[0], recv1.at[0], 0, 16, 9)
    send_ring(send1.at[1], recv1.at[1], 1, 16, 9)
    send_ring(send1.at[1], recv1.at[1], 1, 4, 1)
    for c in range(2):
        send(send1.at[c], recv1.at[c], c, 0, 1 - core)
        keep_own(send1, recv1, c)

    twist = tab[2048:2176, :].astype(F32) + tab[2176:2304, :].astype(F32)
    tc = twist[:rows, :]
    ts = twist[rows:, :]
    row_hi = tab[2304:2432, 256:384]
    row_lo = tab[2432:2560, 256:384]
    low = lax.broadcasted_iota(jnp.int32, (256, 128), 1) < 64
    for c in range(2):
        arrived(recv1.at[c], c)
        if c == 1:
            send_ring(send2.at[0], recv2.at[0], 2, 6, 1)
            send(send2.at[0], recv2.at[0], 2, 0, 1 - core)
        base = c * 512
        spread[base : base + 512, :] = decode(recv1[c].astype(F32).reshape(rows * 8, 128))
        parts = []
        for part in range(2):
            parts.append(
                jnp.concatenate(
                    [spread[pl.ds(base + 4 * part + q, rows, stride=8), :] for q in range(4)], axis=1
                )
            )
        hi, lo = halves(jnp.concatenate(parts, axis=0))
        first = dot(row_hi, hi) + dot(row_hi, lo) + dot(row_lo, hi)
        re = first[:rows, :]
        im = first[rows:, :]
        re_hi, re_lo = halves(tc * re + ts * im)
        im_hi, im_lo = halves(tc * im - ts * re)
        res = dot_t(tab[512:1024, :], jnp.concatenate([re_hi, re_hi], axis=0))
        res = res + dot_t(tab[1536:2048, :], jnp.concatenate([im_hi, im_hi], axis=0))
        both = dot_t(tab[0:512, :], jnp.concatenate([re_hi, re_hi, re_lo, re_lo], axis=0))
        both = both + dot_t(tab[1024:1536, :], jnp.concatenate([im_hi, im_hi, im_lo, im_lo], axis=0))
        spread2[...] = res + both[:, :128] + both[:, 128:]
        paired = jnp.where(low, spread2[pl.ds(0, 256, stride=2), :], spread2[pl.ds(1, 256, stride=2), :])
        send2[c] = paired.reshape(rows // 2, 2, 4, 128).astype(BF16)
        send_ring(send2.at[c], recv2.at[c], 2 + c, 16, 1 if c else 7)
        keep_own(send2, recv2, c)

    send(send2.at[1], recv2.at[1], 3, 0, 1 - core)
    for c in range(2):
        arrived(recv2.at[c], 2 + c)
        spread2[c * 256 : (c + 1) * 256, :] = recv2[c].astype(F32).reshape(rows * 4, 128)
    for pair in range(4):
        turned = jnp.concatenate(
            [spread2[pl.ds(c * 256 + pair, rows, stride=4), :] for c in range(2)], axis=0
        ).T
        out_ref[pair * 128 : (pair + 1) * 128, :] = turned.astype(BF16)
    for c in range(2):
        departed(recv1.at[c], c)
        departed(recv2.at[c], 2 + c)


def body(tokens, out_weight):
    rows = lax.axis_size("row")
    seg_rows = tokens.shape[0]
    operands = [tokens, out_weight, jnp.asarray(make_tables(rows, seg_rows))]
    scratch = [pltpu.VMEM(a.shape, a.dtype) for a in operands]
    scratch += [
        pltpu.VMEM((2048, 512), BF16),
        pltpu.VMEM((rows * 16, 128), F32),
        pltpu.VMEM((2, rows // 2, 2, 8, 128), BF16),
        pltpu.VMEM((2, rows, 8, 128), BF16),
        pltpu.VMEM((2, rows // 2, 2, 4, 128), BF16),
        pltpu.VMEM((2, rows, 4, 128), BF16),
        pltpu.VMEM((rows * 8, 128), F32),
        pltpu.SemaphoreType.DMA((5,)),
        pltpu.SemaphoreType.DMA((4,)),
        pltpu.SemaphoreType.DMA((4,)),
        pltpu.SemaphoreType.REGULAR,
    ]
    return pl.pallas_call(
        functools.partial(kernel, rows),
        out_shape=jax.ShapeDtypeStruct((seg_rows, out_weight.shape[1]), BF16),
        in_specs=[pl.BlockSpec(memory_space=pl.ANY)] * len(operands),
        out_specs=pl.BlockSpec(memory_space=pltpu.VMEM),
        scratch_shapes=scratch,
        compiler_params=pltpu.CompilerParams(
            collective_id=0, has_side_effects=True, vmem_limit_bytes=54848 * 1024
        ),
        name="mix",
    )(*operands)


def solution(mesh):
    placed = (P("row", None), P(None, "col"))
    return jax.shard_map(
        body, mesh=mesh, in_specs=placed, out_specs=P("row", "col"), check_vma=False
    )
```

```python
import functools
import math

import jax
import jax.numpy as jnp
import numpy as np
from jax import lax
from jax.experimental import pallas as pl
from jax.experimental.pallas import tpu as pltpu
from jax.sharding import PartitionSpec as P

GROUPS = 4
GROUP_DIM = 512
MESH_ID = pl.DeviceIdType.MESH
BF16 = jnp.bfloat16
F32 = jnp.float32

FLOOR = 2.0**-6
LIMIT = 34800.0
SHIFT = 125.0 * math.log(2.0)
GAIN = (88.0 + SHIFT) / math.log1p(LIMIT / FLOOR)


def split_table(table):
    hi = table.astype(np.float32).astype(jnp.bfloat16)
    lo = (table - hi.astype(np.float64)).astype(np.float32).astype(jnp.bfloat16)
    return hi, lo


def make_tables(row_count, seg_rows):
    length = row_count * seg_rows
    idx = np.arange(seg_rows)
    phase = (idx[:, None] * idx[None, :]) % seg_rows * (2 * np.pi / seg_rows)
    cos_hi, cos_lo = split_table(np.cos(phase))
    sin_hi, sin_lo = split_table(np.sin(phase))
    row = np.arange(row_count)
    phase = (row[:, None] * row[None, :]) % row_count * (2 * np.pi / row_count)
    cos, sin = np.cos(phase), np.sin(phase)
    row_hi, row_lo = split_table(np.block([[cos, sin], [-sin, cos]]))
    phase = (row[:, None] * idx[None, :]) % length * (2 * np.pi / length)
    scaling = 1.0 / math.sqrt(length * GROUP_DIM)
    twist_hi, twist_lo = split_table(np.concatenate([np.cos(phase), np.sin(phase)], axis=0) * scaling)
    mixed = np.zeros((256, 512), jnp.bfloat16)
    for part in range(2):
        for chan in range(2):
            mixed[128 * chan + 2 * row + part, part * 128 + chan * 64 + row] = 1.0
    mixed[:, 256:384] = np.concatenate([row_hi, row_lo], axis=0)
    return np.concatenate([cos_hi, cos_lo, sin_hi, sin_lo, twist_hi, twist_lo, mixed], axis=0)


def dot(a, b):
    return jnp.dot(a, b, preferred_element_type=F32)


def dot_t(a, b):
    return lax.dot_general(a, b, (((1,), (1,)), ((), ())), preferred_element_type=F32)


def halves(value):
    hi = value.astype(BF16)
    return hi, (value - hi.astype(F32)).astype(BF16)


def encode(value):
    size = jnp.exp(GAIN * jnp.log(1.0 + jnp.abs(value) * (1.0 / FLOOR)) - SHIFT)
    return jnp.where(value < 0.0, -size, size)


def decode(coded):
    size = FLOOR * (jnp.exp((jnp.log(jnp.abs(coded)) + SHIFT) * (1.0 / GAIN)) - 1.0)
    return jnp.where(coded < 0.0, -size, size)


def kernel(
    rows,
    x_hbm, w_hbm, tab_hbm, out_ref,
    x, w, tab, fold, spread, send1, recv1, send2, recv2, spread2,
    load_sem, send_sem, recv_sem, word_sem,
):
    me = lax.axis_index("row")
    col = lax.axis_index("col")
    chips = rows // 2
    chip = me // 2
    core = lax.rem(me, 2)

    loads = []
    for i, (src, dst) in enumerate(
        [
            (w_hbm, w),
            (tab_hbm.at[0:1024], tab.at[0:1024]),
            (tab_hbm.at[1024:2048], tab.at[1024:2048]),
            (x_hbm, x),
            (tab_hbm.at[2048:2560], tab.at[2048:2560]),
        ]
    ):
        load = pltpu.make_async_copy(src, dst, load_sem.at[i])
        load.start()
        loads.append(load)

    barrier = pltpu.get_barrier_semaphore()
    reach = chips // 4

    def place(step, target_core):
        return lax.rem(chip + step + chips, chips) * 2 + target_core

    def signal(sem, step, target_core):
        pl.semaphore_signal(
            sem, inc=1, device_id=(place(step, target_core), col), device_id_type=MESH_ID
        )

    signal(barrier, 0, 1 - core)

    def greet(i, carry):
        for step in (reach - i, i - reach):
            signal(barrier, step, core)
            signal(barrier, step, 1 - core)
        return carry

    lax.fori_loop(0, reach, greet, 0)

    def known_near():
        pl.semaphore_wait(barrier, 4 * reach + 1)
        signal(word_sem, reach, core)
        signal(word_sem, -reach, core)

    def known_all():
        pl.semaphore_wait(word_sem, 2)

    def send(src, dst, which, step, target_core):
        target_chip = lax.rem(chip + step + chips, chips)
        pltpu.make_async_remote_copy(
            src_ref=src.at[target_chip, target_core],
            dst_ref=dst.at[me],
            send_sem=send_sem.at[which],
            recv_sem=recv_sem.at[which],
            device_id=(target_chip * 2 + target_core, col),
            device_id_type=MESH_ID,
        ).start()

    def send_ring(src, dst, which, far, near):
        if far == chips // 2:
            send(src, dst, which, far, core)
            send(src, dst, which, far, 1 - core)
            far -= 1

        def ring(i, carry):
            hop = far - i
            for target_core in (core, 1 - core):
                send(src, dst, which, hop, target_core)
                send(src, dst, which, -hop, target_core)
            return carry

        lax.fori_loop(0, far - near + 1, ring, 0)

    def keep_own(src, dst, c):
        dst[c, pl.ds(me, 1)] = src[c, pl.ds(chip, 1), pl.ds(core, 1)][0]

    def arrived(dst, which):
        part = dst.at[pl.ds(0, rows - 1)]
        pltpu.make_async_copy(part, part, recv_sem.at[which]).wait()

    def departed(dst, which):
        part = dst.at[pl.ds(0, rows - 1)]
        pltpu.make_async_copy(part, part, send_sem.at[which]).wait()

    loads[0].wait()
    wide = jnp.concatenate([w[g * 512 : (g + 1) * 512, :] for g in range(GROUPS)], axis=1)
    for part in range(2):
        loads[1 + part].wait()
        base = part * 1024
        folded = dot(tab[base : base + 512, :], wide) + dot(tab[base + 512 : base + 1024, :], wide)
        hi, lo = halves(-folded if part else folded)
        for g in range(GROUPS):
            fold[g * 512 : (g + 1) * 512, part * 128 : (part + 1) * 128] = hi[:, g * 128 : (g + 1) * 128]
            fold[g * 512 : (g + 1) * 512, 256 + part * 128 : 256 + (part + 1) * 128] = lo[:, g * 128 : (g + 1) * 128]

    loads[3].wait()
    both = dot(x[...], fold[...])
    coded = encode(both[:, :256] + both[:, 256:]).astype(BF16)
    loads[4].wait()
    for q in range(4):
        turned = dot_t(tab[2304:2560, 0:256], coded[q * 128 : (q + 1) * 128, :])
        spread[pl.ds(q, 256, stride=4), :] = turned
    send1[...] = spread[...].astype(BF16).reshape(2, rows // 2, 2, 8, 128)

    known_near()
    send_ring(send1.at[0], recv1.at[0], 0, 8, 1)
    send_ring(send1.at[1], recv1.at[1], 1, 8, 5)
    known_all()
    send_ring(send1.at[0], recv1.at[0], 0, 16, 9)
    send_ring(send1.at[1], recv1.at[1], 1, 16, 9)
    send_ring(send1.at[1], recv1.at[1], 1, 4, 1)
    for c in range(2):
        send(send1.at[c], recv1.at[c], c, 0, 1 - core)
        keep_own(send1, recv1, c)

    twist = tab[2048:2176, :].astype(F32) + tab[2176:2304, :].astype(F32)
    tc = twist[:rows, :]
    ts = twist[rows:, :]
    row_hi = tab[2304:2432, 256:384]
    row_lo = tab[2432:2560, 256:384]
    low = lax.broadcasted_iota(jnp.int32, (256, 128), 1) < 64
    for c in range(2):
        arrived(recv1.at[c], c)
        base = c * 512
        spread[base : base + 512, :] = decode(recv1[c].astype(F32).reshape(rows * 8, 128))
        parts = []
        for part in range(2):
            parts.append(
                jnp.concatenate(
                    [spread[pl.ds(base + 4 * part + q, rows, stride=8), :] for q in range(4)], axis=1
                )
            )
        hi, lo = halves(jnp.concatenate(parts, axis=0))
        first = dot(row_hi, hi) + dot(row_hi, lo) + dot(row_lo, hi)
        re = first[:rows, :]
        im = first[rows:, :]
        re_hi, re_lo = halves(tc * re + ts * im)
        im_hi, im_lo = halves(tc * im - ts * re)
        res = dot_t(tab[512:1024, :], jnp.concatenate([re_hi, re_hi], axis=0))
        res = res + dot_t(tab[1536:2048, :], jnp.concatenate([im_hi, im_hi], axis=0))
        both = dot_t(tab[0:512, :], jnp.concatenate([re_hi, re_hi, re_lo, re_lo], axis=0))
        both = both + dot_t(tab[1024:1536, :], jnp.concatenate([im_hi, im_hi, im_lo, im_lo], axis=0))
        spread2[...] = res + both[:, :128] + both[:, 128:]
        paired = jnp.where(low, spread2[pl.ds(0, 256, stride=2), :], spread2[pl.ds(1, 256, stride=2), :])
        send2[c] = paired.reshape(rows // 2, 2, 4, 128).astype(BF16)
        send_ring(send2.at[c], recv2.at[c], 2 + c, 16, 1 if c else 7)
        keep_own(send2, recv2, c)

    send_ring(send2.at[0], recv2.at[0], 2, 6, 1)
    send(send2.at[0], recv2.at[0], 2, 0, 1 - core)
    send(send2.at[1], recv2.at[1], 3, 0, 1 - core)
    for c in range(2):
        arrived(recv2.at[c], 2 + c)
        spread2[c * 256 : (c + 1) * 256, :] = recv2[c].astype(F32).reshape(rows * 4, 128)
    for pair in range(4):
        turned = jnp.concatenate(
            [spread2[pl.ds(c * 256 + pair, rows, stride=4), :] for c in range(2)], axis=0
        ).T
        out_ref[pair * 128 : (pair + 1) * 128, :] = turned.astype(BF16)
    for c in range(2):
        departed(recv1.at[c], c)
        departed(recv2.at[c], 2 + c)


def body(tokens, out_weight):
    rows = lax.axis_size("row")
    seg_rows = tokens.shape[0]
    operands = [tokens, out_weight, jnp.asarray(make_tables(rows, seg_rows))]
    scratch = [pltpu.VMEM(a.shape, a.dtype) for a in operands]
    scratch += [
        pltpu.VMEM((2048, 512), BF16),
        pltpu.VMEM((rows * 16, 128), F32),
        pltpu.VMEM((2, rows // 2, 2, 8, 128), BF16),
        pltpu.VMEM((2, rows, 8, 128), BF16),
        pltpu.VMEM((2, rows // 2, 2, 4, 128), BF16),
        pltpu.VMEM((2, rows, 4, 128), BF16),
        pltpu.VMEM((rows * 8, 128), F32),
        pltpu.SemaphoreType.DMA((5,)),
        pltpu.SemaphoreType.DMA((4,)),
        pltpu.SemaphoreType.DMA((4,)),
        pltpu.SemaphoreType.REGULAR,
    ]
    return pl.pallas_call(
        functools.partial(kernel, rows),
        out_shape=jax.ShapeDtypeStruct((seg_rows, out_weight.shape[1]), BF16),
        in_specs=[pl.BlockSpec(memory_space=pl.ANY)] * len(operands),
        out_specs=pl.BlockSpec(memory_space=pltpu.VMEM),
        scratch_shapes=scratch,
        compiler_params=pltpu.CompilerParams(
            collective_id=0, has_side_effects=True, vmem_limit_bytes=54848 * 1024
        ),
        name="mix",
    )(*operands)


def solution(mesh):
    placed = (P("row", None), P(None, "col"))
    return jax.shard_map(
        body, mesh=mesh, in_specs=placed, out_specs=P("row", "col"), check_vma=False
    )
```

```python
import functools
import math

import jax
import jax.numpy as jnp
import numpy as np
from jax import lax
from jax.experimental import pallas as pl
from jax.experimental.pallas import tpu as pltpu
from jax.sharding import PartitionSpec as P

GROUPS = 4
GROUP_DIM = 512
MESH_ID = pl.DeviceIdType.MESH
BF16 = jnp.bfloat16
F32 = jnp.float32

FLOOR = 2.0**-6
LIMIT = 34800.0
SHIFT = 125.0 * math.log(2.0)
GAIN = (88.0 + SHIFT) / math.log1p(LIMIT / FLOOR)


def split_table(table):
    hi = table.astype(np.float32).astype(jnp.bfloat16)
    lo = (table - hi.astype(np.float64)).astype(np.float32).astype(jnp.bfloat16)
    return hi, lo


def make_tables(row_count, seg_rows):
    length = row_count * seg_rows
    idx = np.arange(seg_rows)
    phase = (idx[:, None] * idx[None, :]) % seg_rows * (2 * np.pi / seg_rows)
    cos_hi, cos_lo = split_table(np.cos(phase))
    sin_hi, sin_lo = split_table(np.sin(phase))
    row = np.arange(row_count)
    phase = (row[:, None] * row[None, :]) % row_count * (2 * np.pi / row_count)
    cos, sin = np.cos(phase), np.sin(phase)
    row_hi, row_lo = split_table(np.block([[cos, sin], [-sin, cos]]))
    phase = (row[:, None] * idx[None, :]) % length * (2 * np.pi / length)
    scaling = 1.0 / math.sqrt(length * GROUP_DIM)
    twist_hi, twist_lo = split_table(np.concatenate([np.cos(phase), np.sin(phase)], axis=0) * scaling)
    mixed = np.zeros((256, 512), jnp.bfloat16)
    for part in range(2):
        for chan in range(2):
            mixed[128 * chan + 2 * row + part, part * 128 + chan * 64 + row] = 1.0
    mixed[:, 256:384] = np.concatenate([row_hi, row_lo], axis=0)
    return np.concatenate([cos_hi, cos_lo, sin_hi, sin_lo, twist_hi, twist_lo, mixed], axis=0)


def dot(a, b):
    return jnp.dot(a, b, preferred_element_type=F32)


def dot_t(a, b):
    return lax.dot_general(a, b, (((1,), (1,)), ((), ())), preferred_element_type=F32)


def halves(value):
    hi = value.astype(BF16)
    return hi, (value - hi.astype(F32)).astype(BF16)


def encode(value):
    size = jnp.exp(GAIN * jnp.log(1.0 + jnp.abs(value) * (1.0 / FLOOR)) - SHIFT)
    return jnp.where(value < 0.0, -size, size)


def decode(coded):
    size = FLOOR * (jnp.exp((jnp.log(jnp.abs(coded)) + SHIFT) * (1.0 / GAIN)) - 1.0)
    return jnp.where(coded < 0.0, -size, size)


def kernel(
    rows,
    x_hbm, w_hbm, tab_hbm, out_ref,
    x, w, tab, fold, spread, send1, recv1, send2, recv2, spread2,
    load_sem, send_sem, recv_sem, word_sem,
):
    me = lax.axis_index("row")
    col = lax.axis_index("col")
    chips = rows // 2
    chip = me // 2
    core = lax.rem(me, 2)

    loads = []
    for i, (src, dst) in enumerate(
        [
            (w_hbm, w),
            (tab_hbm.at[0:1024], tab.at[0:1024]),
            (tab_hbm.at[1024:2048], tab.at[1024:2048]),
            (x_hbm, x),
            (tab_hbm.at[2048:2560], tab.at[2048:2560]),
        ]
    ):
        load = pltpu.make_async_copy(src, dst, load_sem.at[i])
        load.start()
        loads.append(load)

    barrier = pltpu.get_barrier_semaphore()
    reach = chips // 4

    def place(step, target_core):
        return lax.rem(chip + step + chips, chips) * 2 + target_core

    def signal(sem, step, target_core):
        pl.semaphore_signal(
            sem, inc=1, device_id=(place(step, target_core), col), device_id_type=MESH_ID
        )

    signal(barrier, 0, 1 - core)

    def greet(i, carry):
        for step in (reach - i, i - reach):
            signal(barrier, step, core)
            signal(barrier, step, 1 - core)
        return carry

    lax.fori_loop(0, reach, greet, 0)

    def known_near():
        pl.semaphore_wait(barrier, 4 * reach + 1)
        signal(word_sem, reach, core)
        signal(word_sem, -reach, core)

    def known_all():
        pl.semaphore_wait(word_sem, 2)

    def send(src, dst, which, step, target_core):
        target_chip = lax.rem(chip + step + chips, chips)
        pltpu.make_async_remote_copy(
            src_ref=src.at[target_chip, target_core],
            dst_ref=dst.at[me],
            send_sem=send_sem.at[which],
            recv_sem=recv_sem.at[which],
            device_id=(target_chip * 2 + target_core, col),
            device_id_type=MESH_ID,
        ).start()

    def send_ring(src, dst, which, far, near):
        if far == chips // 2:
            send(src, dst, which, far, core)
            send(src, dst, which, far, 1 - core)
            far -= 1

        def ring(i, carry):
            hop = far - i
            for target_core in (core, 1 - core):
                send(src, dst, which, hop, target_core)
                send(src, dst, which, -hop, target_core)
            return carry

        lax.fori_loop(0, far - near + 1, ring, 0)

    def keep_own(src, dst, c):
        dst[c, pl.ds(me, 1)] = src[c, pl.ds(chip, 1), pl.ds(core, 1)][0]

    def arrived(dst, which):
        part = dst.at[pl.ds(0, rows - 1)]
        pltpu.make_async_copy(part, part, recv_sem.at[which]).wait()

    def departed(dst, which):
        part = dst.at[pl.ds(0, rows - 1)]
        pltpu.make_async_copy(part, part, send_sem.at[which]).wait()

    loads[0].wait()
    wide = jnp.concatenate([w[g * 512 : (g + 1) * 512, :] for g in range(GROUPS)], axis=1)
    for part in range(2):
        loads[1 + part].wait()
        base = part * 1024
        folded = dot(tab[base : base + 512, :], wide) + dot(tab[base + 512 : base + 1024, :], wide)
        hi, lo = halves(-folded if part else folded)
        for g in range(GROUPS):
            fold[g * 512 : (g + 1) * 512, part * 128 : (part + 1) * 128] = hi[:, g * 128 : (g + 1) * 128]
            fold[g * 512 : (g + 1) * 512, 256 + part * 128 : 256 + (part + 1) * 128] = lo[:, g * 128 : (g + 1) * 128]

    loads[3].wait()
    both = dot(x[...], fold[...])
    coded = encode(both[:, :256] + both[:, 256:]).astype(BF16)
    loads[4].wait()
    for q in range(4):
        turned = dot_t(tab[2304:2560, 0:256], coded[q * 128 : (q + 1) * 128, :])
        spread[pl.ds(q, 256, stride=4), :] = turned
    send1[...] = spread[...].astype(BF16).reshape(2, rows // 2, 2, 8, 128)

    known_near()
    send_ring(send1.at[0], recv1.at[0], 0, 8, 1)
    send_ring(send1.at[1], recv1.at[1], 1, 8, 5)
    known_all()
    send_ring(send1.at[0], recv1.at[0], 0, 16, 9)
    send_ring(send1.at[1], recv1.at[1], 1, 16, 9)
    send_ring(send1.at[1], recv1.at[1], 1, 4, 1)
    for c in range(2):
        send(send1.at[c], recv1.at[c], c, 0, 1 - core)
        keep_own(send1, recv1, c)

    twist = tab[2048:2176, :].astype(F32) + tab[2176:2304, :].astype(F32)
    tc = twist[:rows, :]
    ts = twist[rows:, :]
    row_hi = tab[2304:2432, 256:384]
    row_lo = tab[2432:2560, 256:384]
    low = lax.broadcasted_iota(jnp.int32, (256, 128), 1) < 64
    for c in range(2):
        arrived(recv1.at[c], c)
        base = c * 512
        spread[base : base + 512, :] = decode(recv1[c].astype(F32).reshape(rows * 8, 128))
        parts = []
        for part in range(2):
            parts.append(
                jnp.concatenate(
                    [spread[pl.ds(base + 4 * part + q, rows, stride=8), :] for q in range(4)], axis=1
                )
            )
        hi, lo = halves(jnp.concatenate(parts, axis=0))
        first = dot(row_hi, hi) + dot(row_hi, lo) + dot(row_lo, hi)
        re = first[:rows, :]
        im = first[rows:, :]
        re_hi, re_lo = halves(tc * re + ts * im)
        im_hi, im_lo = halves(tc * im - ts * re)
        res = dot_t(tab[512:1024, :], jnp.concatenate([re_hi, re_hi], axis=0))
        res = res + dot_t(tab[1536:2048, :], jnp.concatenate([im_hi, im_hi], axis=0))
        both = dot_t(tab[0:512, :], jnp.concatenate([re_hi, re_hi, re_lo, re_lo], axis=0))
        both = both + dot_t(tab[1024:1536, :], jnp.concatenate([im_hi, im_hi, im_lo, im_lo], axis=0))
        spread2[...] = res + both[:, :128] + both[:, 128:]
        paired = jnp.where(low, spread2[pl.ds(0, 256, stride=2), :], spread2[pl.ds(1, 256, stride=2), :])
        send2[c] = paired.reshape(rows // 2, 2, 4, 128).astype(BF16)
        send_ring(send2.at[c], recv2.at[c], 2 + c, 16, 1 if c else 5)
        keep_own(send2, recv2, c)

    send_ring(send2.at[0], recv2.at[0], 2, 4, 1)
    send(send2.at[0], recv2.at[0], 2, 0, 1 - core)
    send(send2.at[1], recv2.at[1], 3, 0, 1 - core)
    for c in range(2):
        arrived(recv2.at[c], 2 + c)
        spread2[c * 256 : (c + 1) * 256, :] = recv2[c].astype(F32).reshape(rows * 4, 128)
    for pair in range(4):
        turned = jnp.concatenate(
            [spread2[pl.ds(c * 256 + pair, rows, stride=4), :] for c in range(2)], axis=0
        ).T
        out_ref[pair * 128 : (pair + 1) * 128, :] = turned.astype(BF16)
    for c in range(2):
        departed(recv1.at[c], c)
        departed(recv2.at[c], 2 + c)


def body(tokens, out_weight):
    rows = lax.axis_size("row")
    seg_rows = tokens.shape[0]
    operands = [tokens, out_weight, jnp.asarray(make_tables(rows, seg_rows))]
    scratch = [pltpu.VMEM(a.shape, a.dtype) for a in operands]
    scratch += [
        pltpu.VMEM((2048, 512), BF16),
        pltpu.VMEM((rows * 16, 128), F32),
        pltpu.VMEM((2, rows // 2, 2, 8, 128), BF16),
        pltpu.VMEM((2, rows, 8, 128), BF16),
        pltpu.VMEM((2, rows // 2, 2, 4, 128), BF16),
        pltpu.VMEM((2, rows, 4, 128), BF16),
        pltpu.VMEM((rows * 8, 128), F32),
        pltpu.SemaphoreType.DMA((5,)),
        pltpu.SemaphoreType.DMA((4,)),
        pltpu.SemaphoreType.DMA((4,)),
        pltpu.SemaphoreType.REGULAR,
    ]
    return pl.pallas_call(
        functools.partial(kernel, rows),
        out_shape=jax.ShapeDtypeStruct((seg_rows, out_weight.shape[1]), BF16),
        in_specs=[pl.BlockSpec(memory_space=pl.ANY)] * len(operands),
        out_specs=pl.BlockSpec(memory_space=pltpu.VMEM),
        scratch_shapes=scratch,
        compiler_params=pltpu.CompilerParams(
            collective_id=0, has_side_effects=True, vmem_limit_bytes=54848 * 1024
        ),
        name="mix",
    )(*operands)


def solution(mesh):
    placed = (P("row", None), P(None, "col"))
    return jax.shard_map(
        body, mesh=mesh, in_specs=placed, out_specs=P("row", "col"), check_vma=False
    )
```
